32 devices in a mesh: sp: 16 (over z, y, x), tp: 2 (over core).
Axes of the slice: x: 2, y: 2, z: 4, core: 2. Of those that a mesh axis runs over, the one named last changes fastest.
Arguments:
- tokens: bfloat16 [6144, 2048], P('sp', 'tp'), may hold values from -1620 to 1620
- input_norm_gain: float32 [2048], replicated, may hold values from 0.1 to 1.9
- outer_gate_weight: bfloat16 [2048, 1024], P(None, 'tp'), may hold values from -0.125 to 0.125
- inner_gate_weight: bfloat16 [2048, 1024], P(None, 'tp'), may hold values from -0.125 to 0.125
- convolution_input_weight: bfloat16 [2048, 1024], P(None, 'tp'), may hold values from -0.125 to 0.125
- convolution_kernel_taps: bfloat16 [3, 1024], P(None, 'tp'), may hold values from -3 to 3
- query_weight_matrix: bfloat16 [2048, 512], P(None, 'tp'), may hold values from -0.125 to 0.125
- key_weight_matrix: bfloat16 [2048, 512], P(None, 'tp'), may hold values from -0.125 to 0.125
- value_weight_matrix: bfloat16 [2048, 1024], P(None, 'tp'), may hold values from -0.125 to 0.125
- forget_gate_weight: bfloat16 [2048, 512], P(None, 'tp'), may hold values from -0.125 to 0.125
- attention_gate_weight: bfloat16 [2048, 1024], P(None, 'tp'), may hold values from -0.125 to 0.125
- forget_gate_bias: float32 [512], P('tp'), may hold values from -1.5 to 10
- extra_logarithm_decay: float32 [6144, 16], P('sp', 'tp'), may hold values from -0.72 to 0
- initial_head_state: float32 [16, 32, 64], P('tp'), may hold values from -768 to 768
- head_norm_gain: float32 [64], replicated, may hold values from 0.1 to 1.9
- convolution_output_weight: bfloat16 [1024, 2048], P('tp'), may hold values from -0.125 to 0.125
- attention_output_weight: bfloat16 [1024, 2048], P('tp'), may hold values from -0.125 to 0.125
Outputs:
- mixed: bfloat16 [6144, 2048], P(('sp', 'tp'))
The draws below stay inside these ranges and needn't reach their ends.
All inputs are finite; a program needn't handle non-finite values.
Results may differ from the reference program's by a relative error of at most 0.017.
Values may be sent and summed in bfloat16 or wider, within the bound.
A program may use at most 128 MiB of HBM per device.

```python
import math
import jax
import jax.numpy as jnp
from jax import lax

D = 2048
CW = 1024
HEADS = 16
DK = 32
DV = 64
CONV_K = 3
BLOCK = 64
TOK_DEV = 384
TOKENS = 6144


def draw_tokens(key, part):
    noise_key, row_key, col_key = jax.random.split(jax.random.fold_in(key, 11), 3)
    noise = jax.random.truncated_normal(noise_key, -6.0, 6.0, (TOKENS, D), jnp.float32)
    row_scale = jnp.exp(jax.random.uniform(row_key, (TOKENS, 1), jnp.float32) * math.log(10.0))
    ramp = jnp.arange(D, dtype=jnp.float32) / max(D - 1, 1)
    rise = math.log(3.0)
    col_scale = jnp.exp(rise * ramp[None, :] + jax.random.uniform(col_key, (1, D), jnp.float32) * math.log(3.0))
    return (noise * row_scale * col_scale).astype(jnp.bfloat16)


def draw_forget_gate_bias(key, part):
    kind_key, slow_key, fast_key, jitter_key = jax.random.split(jax.random.fold_in(key, 23), 4)
    order = jax.random.permutation(kind_key, HEADS)
    fast_count = HEADS // 2
    is_fast = (order < fast_count)[:, None]
    slow = jax.random.uniform(slow_key, (HEADS, 1), jnp.float32, 8.0, 9.5)
    fast = jax.random.uniform(fast_key, (HEADS, 1), jnp.float32, -1.0, 1.0)
    jitter = jax.random.uniform(jitter_key, (HEADS, DK), jnp.float32, -0.5, 0.5)
    return (jnp.where(is_fast, fast, slow) + jitter).reshape(HEADS * DK)


def draw_extra_logarithm_decay(key, part):
    rate_key, hit_key, size_key = jax.random.split(jax.random.fold_in(key, 37), 3)
    device_blocks = TOKENS // TOK_DEV
    spread = jax.random.uniform(rate_key, (device_blocks, HEADS), jnp.float32) * math.log(4.0)
    per_row = jnp.repeat(5e-06 * jnp.exp(spread), TOK_DEV, axis=0)
    hits = jax.random.randint(hit_key, (TOKENS, HEADS), 0, TOKENS) < 2
    sizes = jax.random.uniform(size_key, (TOKENS, HEADS), jnp.float32, math.log(0.5), math.log(0.8))
    return -per_row + jnp.where(hits, sizes, 0.0)


def block_scale(rng, dims, pieces, least, top_value):
    gain = 1.0
    for axis_at, parts in pieces:
        heights = jax.random.uniform(jax.random.fold_in(jax.random.fold_in(rng, 6), axis_at), (parts,), jnp.float32, least / len(pieces), top_value / len(pieces))
        gain = gain * jnp.repeat(jnp.exp(heights), dims[axis_at] // parts).reshape((-1,) + (1,) * (len(dims) - 1 - axis_at))
    return gain


def bell_draw(rng, shape, deviation, most, cuts=(), kind=jnp.bfloat16):
    level = block_scale(rng, shape, cuts, -0.22, 0.18) if cuts else 1.0
    result = jax.random.normal(rng, shape, jnp.float32) * deviation * level
    return jnp.minimum(jnp.maximum(result, -most), most).astype(kind)


def setup_inputs(seed: int = 0) -> dict:
    seeds = jax.random.split(jax.random.key(seed), 18)
    return {
        "tokens": draw_tokens(jax.random.fold_in(seeds[17], 71), 0),
        "input_norm_gain": jnp.clip(1.0 + 0.18 * jax.random.normal(seeds[1], (D,), jnp.float32), 0.1, 1.9),
        "outer_gate_weight": bell_draw(seeds[2], (D, CW), D ** -0.5, 0.125, ((1, 2),)),
        "inner_gate_weight": bell_draw(seeds[3], (D, CW), D ** -0.5, 0.125, ((1, 2),)),
        "convolution_input_weight": bell_draw(seeds[4], (D, CW), D ** -0.5, 0.125, ((1, 2),)),
        "convolution_kernel_taps": bell_draw(seeds[5], (CONV_K, CW), 0.577, 3.0, ((1, 2),)),
        "query_weight_matrix": bell_draw(seeds[6], (D, HEADS * DK), D ** -0.5, 0.125, ((1, 2),)),
        "key_weight_matrix": bell_draw(seeds[7], (D, HEADS * DK), D ** -0.5, 0.125, ((1, 2),)),
        "value_weight_matrix": bell_draw(seeds[8], (D, HEADS * DV), D ** -0.5, 0.125, ((1, 2),)),
        "forget_gate_weight": bell_draw(seeds[9], (D, HEADS * DK), D ** -0.5, 0.125, ((1, 2),)),
        "attention_gate_weight": bell_draw(seeds[10], (D, HEADS * DV), D ** -0.5, 0.125, ((1, 2),)),
        "forget_gate_bias": draw_forget_gate_bias(jax.random.fold_in(seeds[17], 71), 0),
        "extra_logarithm_decay": draw_extra_logarithm_decay(jax.random.fold_in(seeds[17], 71), 0),
        "initial_head_state": bell_draw(seeds[13], (HEADS, DK, DV), 128.0, 768.0, ((0, 2),), jnp.float32),
        "head_norm_gain": jnp.clip(1.0 + 0.18 * jax.random.normal(seeds[14], (DV,), jnp.float32), 0.1, 1.9),
        "convolution_output_weight": bell_draw(seeds[15], (CW, D), (CW + HEADS * DV) ** -0.5, 0.125, ((0, 2),)),
        "attention_output_weight": bell_draw(seeds[16], (HEADS * DV, D), (CW + HEADS * DV) ** -0.5, 0.125, ((0, 2),)),
    }


NORM_EPS = 1e-06
GATE_SOFTNESS = 16.0

def block_terms(queries, key_rows, values, logarithm_decay):
    cumulative = jnp.cumsum(logarithm_decay, axis=1)
    last_log = cumulative[:, -1:]
    query_g = queries * jnp.exp(cumulative)
    key_g = key_rows * jnp.exp(-cumulative)
    scores = jnp.einsum('nihd,njhd->nhij', query_g, key_g, precision=lax.Precision.HIGHEST)
    width = queries.shape[1]
    causal = jnp.arange(width)[:, None] >= jnp.arange(width)[None, :]
    scores = jnp.where(causal, scores, 0.0)
    inner = jnp.einsum('nhij,njhe->nihe', scores, values, precision=lax.Precision.HIGHEST)
    key_decayed = key_rows * jnp.exp(last_log - cumulative)
    update = jnp.einsum('nchd,nche->nhde', key_decayed, values, precision=lax.Precision.HIGHEST)
    return (query_g, inner, update, last_log[:, 0])

def carry_step(state, inputs):
    block_decay, update = inputs
    return (block_decay[..., None] * state + update, state)

def reference(tokens, input_norm_gain, outer_gate_weight, inner_gate_weight, convolution_input_weight, convolution_kernel_taps, query_weight_matrix, key_weight_matrix, value_weight_matrix, forget_gate_weight, attention_gate_weight, forget_gate_bias, extra_logarithm_decay, initial_head_state, head_norm_gain, convolution_output_weight, attention_output_weight):
    sequence_length = tokens.shape[0]
    number_of_heads, key_channel_count, value_dim = initial_head_state.shape
    features = tokens.astype(jnp.float32)
    power = lax.optimization_barrier(jnp.mean(features * features, axis=1, keepdims=True))
    normed = (features * lax.rsqrt(power + NORM_EPS) * input_norm_gain).astype(jnp.bfloat16)

    def project(weight):
        return jnp.dot(normed, weight, preferred_element_type=jnp.float32).astype(jnp.bfloat16)
    conv_b, conv_c, conv_h = (project(outer_gate_weight), project(inner_gate_weight), project(convolution_input_weight))
    query, key_proj, value = (project(query_weight_matrix), project(key_weight_matrix), project(value_weight_matrix))
    forget_preactivation, out_gate = (project(forget_gate_weight), project(attention_gate_weight))
    product = (conv_c.astype(jnp.float32) * conv_h.astype(jnp.float32)).astype(jnp.bfloat16)
    tap_count = convolution_kernel_taps.shape[0]
    padded = jnp.concatenate([jnp.zeros((tap_count - 1, product.shape[1]), jnp.bfloat16), product], axis=0)
    conv = jnp.zeros(product.shape, jnp.float32)
    for tap_index in range(tap_count):
        conv = conv + convolution_kernel_taps[tap_index].astype(jnp.float32) * padded[tap_index:tap_index + sequence_length].astype(jnp.float32)
    conv_out = (conv_b.astype(jnp.float32) * conv).astype(jnp.bfloat16)
    logarithm_decay = jax.nn.log_sigmoid(forget_preactivation.astype(jnp.float32) + forget_gate_bias) / GATE_SOFTNESS
    logarithm_decay = logarithm_decay.reshape(sequence_length, number_of_heads, key_channel_count) + extra_logarithm_decay[:, :, None]
    n_blocks = sequence_length // BLOCK
    queries = (query.astype(jnp.float32) * key_channel_count ** (-0.5)).reshape(n_blocks, BLOCK, number_of_heads, key_channel_count)
    key_rows = key_proj.astype(jnp.float32).reshape(n_blocks, BLOCK, number_of_heads, key_channel_count)
    values = value.astype(jnp.float32).reshape(n_blocks, BLOCK, number_of_heads, value_dim)
    query_g, inner, update, block_log = block_terms(queries, key_rows, values, logarithm_decay.reshape(n_blocks, BLOCK, number_of_heads, key_channel_count))
    final_state, entering = lax.scan(carry_step, initial_head_state.astype(jnp.float32), (jnp.exp(block_log), update))
    outer = jnp.einsum('nchd,nhde->nche', query_g, entering, precision=lax.Precision.HIGHEST)
    raw = (inner + outer).reshape(sequence_length, number_of_heads, value_dim)
    raw = raw * lax.rsqrt(lax.optimization_barrier(jnp.mean(raw * raw, axis=2, keepdims=True)) + NORM_EPS) * head_norm_gain
    gate_values = jax.nn.silu(out_gate.astype(jnp.float32)).reshape(sequence_length, number_of_heads, value_dim)
    attn_out = (raw * gate_values).reshape(sequence_length, number_of_heads * value_dim).astype(jnp.bfloat16)
    mixed = jnp.dot(conv_out, convolution_output_weight, preferred_element_type=jnp.float32)
    mixed = mixed + jnp.dot(attn_out, attention_output_weight, preferred_element_type=jnp.float32)
    return mixed.astype(jnp.bfloat16)
```

```python
import functools

import jax
import jax.numpy as jnp
from jax import lax
from jax.experimental import pallas as pl
from jax.experimental.pallas import tpu as pltpu
from jax.sharding import PartitionSpec as P

BLOCK = 64
NORM_EPS = 1e-06
GATE_SOFTNESS = 16.0
CHUNK = 256
OUT_CHUNKS = 4
F32, BF16 = jnp.float32, jnp.bfloat16
NT = (((1,), (1,)), ((), ()))
TN = (((0,), (0,)), ((), ()))


def radices(n):
    found = []
    while n > 1:
        r = 4 if n % 4 == 0 else (2 if n % 2 == 0 else n)
        found.append(r)
        n //= r
    return found


def dot32(a, b, dims=(((1,), (0,)), ((), ()))):
    return lax.dot_general(
        a, b, dims, precision=lax.Precision.HIGHEST, preferred_element_type=F32
    )


def dot16(a, b, dims=(((1,), (0,)), ((), ()))):
    return lax.dot_general(a, b, dims, preferred_element_type=F32)


def same_group(shape, row_size, col_size):
    rows = lax.broadcasted_iota(jnp.int32, shape, 0) // row_size
    cols = lax.broadcasted_iota(jnp.int32, shape, 1) // col_size
    return rows == cols


def kernel(n, sizes, *refs):
    rows, feats, heads, dk, dv, cw, widths = sizes
    qk, vw = heads * dk, heads * dv
    (x_ref, gain_ref, wb, wc, wh, taps_ref, wq, wk, wv, wf, wg, bias_ref, extra_ref,
     init_ref, hgain_ref, wco, wao, out_ref,
     wall, wout, nrm, peer, pj, qg_s, kg_s, inner_s, enter_s, excl_s, maskk, maskv,
     prf, halo_s, halo_r, cat, msg, back_s, back_r, wsem, ssem, rsem) = refs
    sp, tp = lax.axis_index("sp"), lax.axis_index("tp")
    levels = radices(n)
    order = (wf, wk, wv, wq, wc, wh, wb, wg)
    loads = []
    at = 0
    offs = []
    for i, (w, width) in enumerate(zip(order, widths)):
        loads.append(pltpu.make_async_copy(w, wall.at[:, at:at + width], wsem.at[i]))
        offs.append(at)
        at += width
    loads.append(pltpu.make_async_copy(wco, wout.at[0:cw, :], wsem.at[8]))
    loads.append(pltpu.make_async_copy(wao, wout.at[cw:cw + vw, :], wsem.at[9]))
    o_f, o_k, o_v, o_q, o_c, o_h, o_b, o_g = offs
    for c in loads[:4]:
        c.start()

    partner = {"tp": 1 - tp}
    nxt = {"sp": lax.rem(sp + 1, n)}
    prv = {"sp": lax.rem(sp + n - 1, n)}
    peers = []
    stride = 1
    for r in levels:
        digit = lax.rem(sp // stride, r)
        base = sp - digit * stride
        peers.append((r, digit, [
            {"sp": base + lax.rem(digit + o, r) * stride} for o in range(1, r)
        ]))
        stride *= r
    everyone = [partner, nxt, prv] + [d for _, _, ds in peers for d in ds]
    barrier = pltpu.get_barrier_semaphore()
    for d in everyone:
        pl.semaphore_signal(barrier, inc=1, device_id=d, device_id_type=pl.DeviceIdType.MESH)
    pl.semaphore_wait(barrier, len(everyone))

    def remote(src, dst, k, device):
        return pltpu.make_async_remote_copy(
            src_ref=src, dst_ref=dst, send_sem=ssem.at[k], recv_sem=rsem.at[k],
            device_id=device, device_id_type=pl.DeviceIdType.MESH,
        )

    swap = remote(x_ref, peer, 0, partner)
    swap.start()
    for c in loads[4:]:
        c.start()

    maskk[...] = jnp.where(same_group(maskk.shape, BLOCK, dk), 1.0, 0.0).astype(BF16)
    maskv[...] = jnp.where(same_group(maskv.shape, BLOCK, dv), 1.0, 0.0).astype(BF16)
    half = feats // 2
    mine = pl.ds(pl.multiple_of(tp * half, half), half)
    theirs = pl.ds(pl.multiple_of((1 - tp) * half, half), half)
    swap.wait()

    def norm_rows(i, carry):
        r = pl.ds(pl.multiple_of(i * 32, 32), 32)
        a, b = x_ref[r, :].astype(F32), peer[r, :].astype(F32)
        power = (
            jnp.sum(a * a, axis=1, keepdims=True) + jnp.sum(b * b, axis=1, keepdims=True)
        ) * (1.0 / feats)
        scale = lax.rsqrt(power + NORM_EPS)
        nrm[r, mine] = (a * scale * gain_ref[:, mine]).astype(BF16)
        nrm[r, theirs] = (b * scale * gain_ref[:, theirs]).astype(BF16)
        return carry

    lax.fori_loop(0, rows // 32, norm_rows, 0)

    def project(first, last):
        def one(i, carry):
            c = pl.ds(pl.multiple_of(i * CHUNK, CHUNK), CHUNK)
            pj[:, c] = dot16(nrm[...], wall[:, c]).astype(BF16)
            return carry

        lax.fori_loop(first // CHUNK, last // CHUNK, one, 0)

    for c in loads[:4]:
        c.wait()
    project(0, o_c)

    n_blocks = rows // BLOCK
    tri_r = lax.broadcasted_iota(jnp.int32, (BLOCK, BLOCK), 0)
    tri_c = lax.broadcasted_iota(jnp.int32, (BLOCK, BLOCK), 1)
    tri = jnp.where(tri_r >= tri_c, 1.0, 0.0)
    spread = jnp.where(same_group((heads, qk), 1, dk), 1.0, 0.0)
    state = jnp.zeros((dv, qk), F32)
    total = jnp.zeros((1, qk), F32)
    for b in range(n_blocks):
        r = slice(b * BLOCK, (b + 1) * BLOCK)
        z = pj[r, o_f:o_f + qk].astype(F32) + bias_ref[...]
        decay = (jnp.minimum(z, 0.0) - jnp.log1p(jnp.exp(-jnp.abs(z)))) * (1.0 / GATE_SOFTNESS)
        decay = decay + dot32(extra_ref[r, :], spread)
        cum = dot32(tri, decay)
        last = cum[BLOCK - 1:BLOCK, :]
        keys = pj[r, o_k:o_k + qk].astype(F32)
        kdec = (keys * jnp.exp(last - cum)).astype(BF16)
        full = dot16(pj[r, o_v:o_v + vw], kdec, TN)
        update = jnp.zeros((dv, qk), F32)
        for h in range(heads):
            s = slice(h * dv, (h + 1) * dv)
            update = update + full[s, :] * maskk[s, :].astype(F32)
        kg_s[r, :] = (keys * jnp.exp(-cum)).astype(BF16)
        qg_s[r, :] = (
            pj[r, o_q:o_q + qk].astype(F32) * dk ** (-0.5) * jnp.exp(cum)
        ).astype(BF16)
        enter_s[b] = state
        excl_s[b] = jnp.broadcast_to(jnp.exp(total), (8, qk))
        state = state * jnp.exp(last) + update
        total = total + last

    pre_s, pre_d = jnp.zeros((dv, qk), F32), jnp.ones((1, qk), F32)
    tot_s, tot_d = state, jnp.exp(total)

    def send_level(lv, tot_s, tot_d):
        r, digit, ds = peers[lv]
        msg[lv, 0, 0:dv, :] = tot_s
        msg[lv, 0, dv:dv + 8, :] = jnp.broadcast_to(tot_d, (8, qk))
        copies = [
            remote(msg.at[lv, 0], msg.at[lv, o], 8 + lv * 4 + o, ds[o - 1]) for o in range(1, r)
        ]
        for c in copies:
            c.start()
        return copies

    def join_level(lv, copies, pre_s, pre_d):
        r, digit, _ = peers[lv]
        for c in copies:
            c.wait()
        low_s, low_d = jnp.zeros((dv, qk), F32), jnp.ones((1, qk), F32)
        all_s, all_d = low_s, low_d
        for j in range(r):
            slot = lax.rem(digit + r - j, r)
            part_s = msg[lv, slot, 0:dv, :]
            part_d = msg[lv, slot, dv:dv + 1, :]
            all_s, all_d = part_d * all_s + part_s, all_d * part_d
            before = j < digit
            low_s = jnp.where(before, all_s, low_s)
            low_d = jnp.where(before, all_d, low_d)
        return all_s, all_d, pre_d * low_s + pre_s, low_d * pre_d

    copies = send_level(0, tot_s, tot_d) if levels else []

    for c in loads[4:8]:
        c.wait()
    project(o_c, o_b)
    for b in range(n_blocks):
        r = slice(b * BLOCK, (b + 1) * BLOCK)
        product = (
            pj[r, o_c:o_c + cw].astype(F32) * pj[r, o_h:o_h + cw].astype(F32)
        ).astype(BF16)
        prf[8 + b * BLOCK:8 + (b + 1) * BLOCK, :] = product.astype(F32)
        if b == n_blocks - 1:
            halo_s[...] = product[BLOCK - 16:, :]
    halo = remote(halo_s, halo_r, 1, nxt)
    halo.start()

    if levels:
        tot_s, tot_d, pre_s, pre_d = join_level(0, copies, pre_s, pre_d)
    if len(levels) > 1:
        copies = send_level(1, tot_s, tot_d)

    project(o_b, o_g + vw)
    causal_r = lax.broadcasted_iota(jnp.int32, (BLOCK, heads * BLOCK), 0)
    causal_c = lax.rem(lax.broadcasted_iota(jnp.int32, (BLOCK, heads * BLOCK), 1), BLOCK)
    causal = causal_r >= causal_c
    for b in range(n_blocks):
        r = slice(b * BLOCK, (b + 1) * BLOCK)
        kst = jnp.concatenate([kg_s[r, :]] * heads, axis=0) * maskk[...]
        scores = jnp.where(causal, dot16(qg_s[r, :], kst, NT), 0.0).astype(BF16)
        vst = jnp.concatenate([pj[r, o_v:o_v + vw]] * heads, axis=0) * maskv[...]
        inner_s[r, :] = dot16(scores, vst)

    halo.wait()
    prf[0:8, :] = jnp.where(sp > 0, halo_r[8:16, :].astype(F32), 0.0)
    taps = taps_ref[...].astype(F32)
    count = taps.shape[0]
    for b in range(n_blocks):
        conv = jnp.zeros((BLOCK, cw), F32)
        for j in range(count):
            start = 8 + b * BLOCK - (count - 1) + j
            conv = conv + taps[j:j + 1, :] * prf[start:start + BLOCK, :]
        r = slice(b * BLOCK, (b + 1) * BLOCK)
        cat[r, 0:cw] = (pj[r, o_b:o_b + cw].astype(F32) * conv).astype(BF16)

    for lv in range(1, len(levels)):
        tot_s, tot_d, pre_s, pre_d = join_level(lv, copies, pre_s, pre_d)
        if lv + 1 < len(levels):
            copies = send_level(lv + 1, tot_s, tot_d)

    eye = jnp.where(
        lax.broadcasted_iota(jnp.int32, (dv, dv), 0)
        == lax.broadcasted_iota(jnp.int32, (dv, dv), 1), 1.0, 0.0)
    incoming = pre_s + pre_d * dot32(eye, init_ref[...], NT)
    repeat = jnp.where(
        lax.broadcasted_iota(jnp.int32, (dv, vw), 0)
        == lax.rem(lax.broadcasted_iota(jnp.int32, (dv, vw), 1), dv), 1.0, 0.0)
    hgain = dot32(jnp.broadcast_to(hgain_ref[...], (8, dv)), repeat)[0:1, :]
    for b in range(n_blocks):
        r = slice(b * BLOCK, (b + 1) * BLOCK)
        entering = (enter_s[b] + excl_s[b, 0:1, :] * incoming).astype(BF16)
        sst = jnp.concatenate([entering] * heads, axis=0) * maskk[...]
        raw = inner_s[r, :] + dot16(qg_s[r, :], sst, NT)
        power = dot16((raw * raw).astype(BF16), maskv[...]) * (1.0 / dv)
        gate = pj[r, o_g:o_g + vw].astype(F32)
        gate = gate / (1.0 + jnp.exp(-gate))
        cat[r, cw:cw + vw] = (raw * lax.rsqrt(power + NORM_EPS) * hgain * gate).astype(BF16)

    for c in loads[8:]:
        c.wait()
    own = rows // 2
    my_rows = pl.ds(pl.multiple_of(tp * own, own), own)
    peer_rows = pl.ds(pl.multiple_of((1 - tp) * own, own), own)
    step = feats // OUT_CHUNKS
    backs = []
    for i in range(OUT_CHUNKS):
        c = slice(i * step, (i + 1) * step)
        back_s[i] = dot16(cat[peer_rows, :], wout[:, c]).astype(BF16)
        backs.append(remote(back_s.at[i], back_r.at[i], 2 + i, partner))
        backs[-1].start()
    for i in range(OUT_CHUNKS):
        c = slice(i * step, (i + 1) * step)
        part = dot16(cat[my_rows, :], wout[:, c])
        backs[i].wait()
        out_ref[:, c] = (part + back_r[i].astype(F32)).astype(BF16)


def on_device(n, tokens, gain, wb, wc, wh, taps, wq, wk, wv, wf, wg, bias, extra, init,
              hgain, wco, wao):
    rows = tokens.shape[0]
    feats = gain.shape[0]
    heads, dk, dv = init.shape
    cw = wb.shape[1]
    qk, vw = heads * dk, heads * dv
    widths = tuple(w.shape[1] for w in (wf, wk, wv, wq, wc, wh, wb, wg))
    sizes = (rows, feats, heads, dk, dv, cw, widths)
    vm, hbm = pl.BlockSpec(memory_space=pltpu.VMEM), pl.BlockSpec(memory_space=pl.ANY)
    n_blocks = rows // BLOCK
    levels = max(len(radices(n)), 1)
    out_rows = rows // 2
    step = feats // OUT_CHUNKS
    n_sems = 8 + 4 * levels
    return pl.pallas_call(
        functools.partial(kernel, n, sizes),
        out_shape=jax.ShapeDtypeStruct((out_rows, feats), BF16),
        in_specs=[vm, vm, hbm, hbm, hbm, vm, hbm, hbm, hbm, hbm, hbm, vm, vm, vm, vm, hbm, hbm],
        out_specs=vm,
        scratch_shapes=[
            pltpu.VMEM((feats, sum(widths)), BF16),
            pltpu.VMEM((cw + vw, feats), BF16),
            pltpu.VMEM((rows, feats), BF16),
            pltpu.VMEM((rows, feats // 2), BF16),
            pltpu.VMEM((rows, sum(widths)), BF16),
            pltpu.VMEM((rows, qk), BF16),
            pltpu.VMEM((rows, qk), BF16),
            pltpu.VMEM((rows, vw), F32),
            pltpu.VMEM((n_blocks, dv, qk), F32),
            pltpu.VMEM((n_blocks, 8, qk), F32),
            pltpu.VMEM((heads * BLOCK, qk), BF16),
            pltpu.VMEM((heads * BLOCK, vw), BF16),
            pltpu.VMEM((rows + 8, cw), F32),
            pltpu.VMEM((16, cw), BF16),
            pltpu.VMEM((16, cw), BF16),
            pltpu.VMEM((rows, cw + vw), BF16),
            pltpu.VMEM((levels, 4, dv + 8, qk), F32),
            pltpu.VMEM((OUT_CHUNKS, out_rows, step), BF16),
            pltpu.VMEM((OUT_CHUNKS, out_rows, step), BF16),
            pltpu.SemaphoreType.DMA((10,)),
            pltpu.SemaphoreType.DMA((n_sems,)),
            pltpu.SemaphoreType.DMA((n_sems,)),
        ],
        compiler_params=pltpu.CompilerParams(
            collective_id=0, has_side_effects=True, vmem_limit_bytes=60 * 2**20
        ),
        name="mixer",
    )(
        tokens, gain.reshape(1, feats), wb, wc, wh, taps, wq, wk, wv, wf, wg,
        bias.reshape(1, qk), extra, init.reshape(qk, dv), hgain.reshape(1, dv), wco, wao,
    )


def solution(mesh):
    placed = (
        P("sp", "tp"), P(), P(None, "tp"), P(None, "tp"), P(None, "tp"), P(None, "tp"),
        P(None, "tp"), P(None, "tp"), P(None, "tp"), P(None, "tp"), P(None, "tp"),
        P("tp"), P("sp", "tp"), P("tp", None, None), P(), P("tp", None), P("tp", None),
    )
    return jax.shard_map(
        functools.partial(on_device, mesh.shape["sp"]), mesh=mesh, in_specs=placed,
        out_specs=P(("sp", "tp"), None), check_vma=False,
    )
```

```python
import functools

import jax
import jax.numpy as jnp
from jax import lax
from jax.experimental import pallas as pl
from jax.experimental.pallas import tpu as pltpu
from jax.sharding import PartitionSpec as P

BLOCK = 64
NORM_EPS = 1e-06
GATE_SOFTNESS = 16.0
CHUNK = 256
OUT_CHUNKS = 4
F32, BF16 = jnp.float32, jnp.bfloat16
NT = (((1,), (1,)), ((), ()))
TN = (((0,), (0,)), ((), ()))


def radices(n):
    found = []
    while n > 1:
        r = 4 if n % 4 == 0 else (2 if n % 2 == 0 else n)
        found.append(r)
        n //= r
    return found


def dot32(a, b, dims=(((1,), (0,)), ((), ()))):
    return lax.dot_general(
        a, b, dims, precision=lax.Precision.HIGHEST, preferred_element_type=F32
    )


def dot16(a, b, dims=(((1,), (0,)), ((), ()))):
    return lax.dot_general(a, b, dims, preferred_element_type=F32)


def same_group(shape, row_size, col_size):
    rows = lax.broadcasted_iota(jnp.int32, shape, 0) // row_size
    cols = lax.broadcasted_iota(jnp.int32, shape, 1) // col_size
    return rows == cols


def kernel(n, sizes, *refs):
    rows, feats, heads, dk, dv, cw, widths = sizes
    qk, vw = heads * dk, heads * dv
    (x_ref, gain_ref, wb, wc, wh, taps_ref, wq, wk, wv, wf, wg, bias_ref, extra_ref,
     init_ref, hgain_ref, wco, wao, out_ref,
     wall, wout, ya, yb, peer, acc, scale_s, ext_s, oacc, pj, qg_s, kg_s, inner_s, enter_s, excl_s, maskk, maskv,
     prf, halo_s, halo_r, cat, msg, back_s, back_r, wsem, ssem, rsem) = refs
    sp, tp = lax.axis_index("sp"), lax.axis_index("tp")
    levels = radices(n)
    order = (wf, wk, wv, wq, wc, wh, wb, wg)
    half = feats // 2
    mine = pl.ds(pl.multiple_of(tp * half, half), half)
    theirs = pl.ds(pl.multiple_of((1 - tp) * half, half), half)
    first, second, offs = [], [], []
    at = 0
    for i, (w, width) in enumerate(zip(order, widths)):
        for j, (part, found) in enumerate(((mine, first), (theirs, second))):
            found.append(pltpu.make_async_copy(
                w.at[part, :], wall.at[part, at:at + width], wsem.at[8 * j + i]))
        offs.append(at)
        at += width
    end = at
    load_co = pltpu.make_async_copy(wco, wout.at[0:cw, :], wsem.at[16])
    load_ao = pltpu.make_async_copy(wao, wout.at[cw:cw + vw, :], wsem.at[17])
    o_f, o_k, o_v, o_q, o_c, o_h, o_b, o_g = offs
    for c in first + second + [load_co, load_ao]:
        c.start()

    partner = {"tp": 1 - tp}
    nxt = {"sp": lax.rem(sp + 1, n)}
    prv = {"sp": lax.rem(sp + n - 1, n)}
    peers = []
    stride = 1
    for r in levels:
        digit = lax.rem(sp // stride, r)
        base = sp - digit * stride
        peers.append((r, digit, [
            {"sp": base + lax.rem(digit + o, r) * stride} for o in range(1, r)
        ]))
        stride *= r
    everyone = [partner] + [d for _, _, ds in peers for d in ds]
    barrier = pltpu.get_barrier_semaphore()
    for d in everyone:
        pl.semaphore_signal(barrier, inc=1, device_id=d, device_id_type=pl.DeviceIdType.MESH)

    def remote(src, dst, k, device):
        return pltpu.make_async_remote_copy(
            src_ref=src, dst_ref=dst, send_sem=ssem.at[k], recv_sem=rsem.at[k],
            device_id=device, device_id_type=pl.DeviceIdType.MESH,
        )

    @pl.when(sp < n - 1)
    def _():
        pl.semaphore_signal(barrier, inc=1, device_id=nxt, device_id_type=pl.DeviceIdType.MESH)

    @pl.when(sp > 0)
    def _():
        pl.semaphore_signal(barrier, inc=1, device_id=prv, device_id_type=pl.DeviceIdType.MESH)

    swap = remote(x_ref, peer, 0, partner)

    def own_rows(i, carry):
        r = pl.ds(pl.multiple_of(i * 32, 32), 32)
        a = x_ref[r, :].astype(F32)
        ya[r, :] = (a * gain_ref[:, mine]).astype(BF16)
        scale_s[r, :] = jnp.broadcast_to(
            jnp.sum(a * a, axis=1, keepdims=True), (32, CHUNK))
        return carry

    def peer_rows_in(i, carry):
        r = pl.ds(pl.multiple_of(i * 32, 32), 32)
        b = peer[r, :].astype(F32)
        yb[r, :] = (b * gain_ref[:, theirs]).astype(BF16)
        power = (scale_s[r, :] + jnp.sum(b * b, axis=1, keepdims=True)) * (1.0 / feats)
        scale_s[r, :] = lax.rsqrt(power + NORM_EPS)
        return carry

    def project_own(lo, hi):
        def one(i, carry):
            c = pl.ds(pl.multiple_of(i * CHUNK, CHUNK), CHUNK)
            acc[:, c] = dot16(ya[...], wall[mine, c])
            return carry

        lax.fori_loop(lo // CHUNK, hi // CHUNK, one, 0, unroll=True)

    def project(lo, hi):
        def one(i, carry):
            c = pl.ds(pl.multiple_of(i * CHUNK, CHUNK), CHUNK)
            whole = acc[:, c] + dot16(yb[...], wall[theirs, c])
            pj[:, c] = (whole * scale_s[...]).astype(BF16)
            return carry

        lax.fori_loop(lo // CHUNK, hi // CHUNK, one, 0, unroll=True)

    lax.fori_loop(0, rows // 32, own_rows, 0)
    for c in first[:4]:
        c.wait()
    project_own(0, o_c)
    ends = jnp.where(sp > 0, 1, 0) + jnp.where(sp < n - 1, 1, 0)
    pl.semaphore_wait(barrier, len(everyone) + ends)
    swap.start()
    for c in first[4:]:
        c.wait()
    project_own(o_c, end)
    maskk[...] = jnp.where(same_group(maskk.shape, BLOCK, dk), 1.0, 0.0).astype(BF16)
    maskv[...] = jnp.where(same_group(maskv.shape, BLOCK, dv), 1.0, 0.0).astype(BF16)
    spread = jnp.where(same_group((heads, qk), 1, dk), 1.0, 0.0)
    ext_s[...] = dot32(extra_ref[...], spread, TN)
    swap.wait()
    lax.fori_loop(0, rows // 32, peer_rows_in, 0)
    for c in second[:4]:
        c.wait()
    project(0, o_c)

    n_blocks = rows // BLOCK
    tri_r = lax.broadcasted_iota(jnp.int32, (BLOCK, BLOCK), 0)
    tri_c = lax.broadcasted_iota(jnp.int32, (BLOCK, BLOCK), 1)
    tri = jnp.where(tri_r >= tri_c, 1.0, 0.0)
    state = jnp.zeros((dv, qk), F32)
    total = jnp.zeros((1, qk), F32)
    for b in range(n_blocks):
        r = slice(b * BLOCK, (b + 1) * BLOCK)
        z = pj[r, o_f:o_f + qk].astype(F32) + bias_ref[...]
        decay = (jnp.minimum(z, 0.0) - jnp.log1p(jnp.exp(-jnp.abs(z)))) * (1.0 / GATE_SOFTNESS)
        decay = decay + ext_s[r, :]
        cum = dot32(tri, decay)
        last = cum[BLOCK - 1:BLOCK, :]
        keys = pj[r, o_k:o_k + qk].astype(F32)
        kdec = (keys * jnp.exp(last - cum)).astype(BF16)
        full = dot16(pj[r, o_v:o_v + vw], kdec, TN)
        update = jnp.zeros((dv, qk), F32)
        for h in range(heads):
            s = slice(h * dv, (h + 1) * dv)
            update = update + full[s, :] * maskk[s, :].astype(F32)
        kg_s[r, :] = (keys * jnp.exp(-cum)).astype(BF16)
        qg_s[r, :] = (
            pj[r, o_q:o_q + qk].astype(F32) * dk ** (-0.5) * jnp.exp(cum)
        ).astype(BF16)
        enter_s[b] = state
        excl_s[b] = jnp.broadcast_to(jnp.exp(total), (8, qk))
        state = state * jnp.exp(last) + update
        total = total + last

    pre_s, pre_d = jnp.zeros((dv, qk), F32), jnp.ones((1, qk), F32)
    tot_s, tot_d = state, jnp.exp(total)

    def send_level(lv, tot_s, tot_d):
        r, digit, ds = peers[lv]
        high = tot_d.astype(BF16).astype(F32)
        msg[lv, 0, 0:dv, :] = tot_s.astype(BF16)
        msg[lv, 0, dv:dv + 16, :] = jnp.concatenate([
            jnp.broadcast_to(high, (8, qk)), jnp.broadcast_to(tot_d - high, (8, qk))
        ], axis=0).astype(BF16)
        copies = [
            remote(msg.at[lv, 0], msg.at[lv, o], 8 + lv * 4 + o, ds[o - 1]) for o in range(1, r)
        ]
        for c in copies:
            c.start()
        return copies

    def join_level(lv, copies, pre_s, pre_d):
        r, digit, _ = peers[lv]
        for c in copies:
            c.wait()
        low_s, low_d = jnp.zeros((dv, qk), F32), jnp.ones((1, qk), F32)
        all_s, all_d = low_s, low_d
        for j in range(r):
            slot = lax.rem(digit + r - j, r)
            part_s = msg[lv, slot, 0:dv, :].astype(F32)
            pair = msg[lv, slot, dv:dv + 16, :].astype(F32)
            part_d = pair[0:1, :] + pair[8:9, :]
            all_s, all_d = part_d * all_s + part_s, all_d * part_d
            before = j < digit
            low_s = jnp.where(before, all_s, low_s)
            low_d = jnp.where(before, all_d, low_d)
        return all_s, all_d, pre_d * low_s + pre_s, low_d * pre_d

    copies = send_level(0, tot_s, tot_d) if levels else []

    for c in second[4:]:
        c.wait()
    project(o_c, o_b)
    for b in range(n_blocks):
        r = slice(b * BLOCK, (b + 1) * BLOCK)
        product = (
            pj[r, o_c:o_c + cw].astype(F32) * pj[r, o_h:o_h + cw].astype(F32)
        ).astype(BF16)
        prf[8 + b * BLOCK:8 + (b + 1) * BLOCK, :] = product.astype(F32)
        if b == n_blocks - 1:
            halo_s[...] = product[BLOCK - 16:, :]
    halo = remote(halo_s, halo_r, 1, nxt)

    @pl.when(sp < n - 1)
    def _():
        halo.start()

    project(o_b, end)

    if levels:
        tot_s, tot_d, pre_s, pre_d = join_level(0, copies, pre_s, pre_d)
    if len(levels) > 1:
        copies = send_level(1, tot_s, tot_d)

    causal_r = lax.broadcasted_iota(jnp.int32, (BLOCK, heads * BLOCK), 0)
    causal_c = lax.rem(lax.broadcasted_iota(jnp.int32, (BLOCK, heads * BLOCK), 1), BLOCK)
    causal = causal_r >= causal_c
    for b in range(n_blocks):
        r = slice(b * BLOCK, (b + 1) * BLOCK)
        kst = jnp.concatenate([kg_s[r, :]] * heads, axis=0) * maskk[...]
        scores = jnp.where(causal, dot16(qg_s[r, :], kst, NT), 0.0).astype(BF16)
        vst = jnp.concatenate([pj[r, o_v:o_v + vw]] * heads, axis=0) * maskv[...]
        inner_s[r, :] = dot16(scores, vst)

    @pl.when(sp < n - 1)
    def _():
        halo.wait_send()

    @pl.when(sp > 0)
    def _():
        halo.wait_recv()
        prf[0:8, :] = halo_r[8:16, :].astype(F32)

    @pl.when(sp == 0)
    def _():
        prf[0:8, :] = jnp.zeros((8, cw), F32)

    taps = taps_ref[...].astype(F32)
    count = taps.shape[0]
    for b in range(n_blocks):
        conv = jnp.zeros((BLOCK, cw), F32)
        for j in range(count):
            start = 8 + b * BLOCK - (count - 1) + j
            conv = conv + taps[j:j + 1, :] * prf[start:start + BLOCK, :]
        r = slice(b * BLOCK, (b + 1) * BLOCK)
        cat[r, 0:cw] = (pj[r, o_b:o_b + cw].astype(F32) * conv).astype(BF16)

    step = feats // OUT_CHUNKS
    load_co.wait()
    for i in range(OUT_CHUNKS):
        c = slice(i * step, (i + 1) * step)
        oacc[:, c] = dot16(cat[:, 0:cw], wout[0:cw, c])

    for lv in range(1, len(levels)):
        tot_s, tot_d, pre_s, pre_d = join_level(lv, copies, pre_s, pre_d)
        if lv + 1 < len(levels):
            copies = send_level(lv + 1, tot_s, tot_d)

    eye = jnp.where(
        lax.broadcasted_iota(jnp.int32, (dv, dv), 0)
        == lax.broadcasted_iota(jnp.int32, (dv, dv), 1), 1.0, 0.0)
    incoming = pre_s + pre_d * dot32(eye, init_ref[...], NT)
    repeat = jnp.where(
        lax.broadcasted_iota(jnp.int32, (dv, vw), 0)
        == lax.rem(lax.broadcasted_iota(jnp.int32, (dv, vw), 1), dv), 1.0, 0.0)
    hgain = dot32(jnp.broadcast_to(hgain_ref[...], (8, dv)), repeat)[0:1, :]
    for b in range(n_blocks):
        r = slice(b * BLOCK, (b + 1) * BLOCK)
        entering = (enter_s[b] + excl_s[b, 0:1, :] * incoming).astype(BF16)
        sst = jnp.concatenate([entering] * heads, axis=0) * maskk[...]
        raw = inner_s[r, :] + dot16(qg_s[r, :], sst, NT)
        power = dot16((raw * raw).astype(BF16), maskv[...]) * (1.0 / dv)
        gate = pj[r, o_g:o_g + vw].astype(F32)
        gate = gate / (1.0 + jnp.exp(-gate))
        cat[r, cw:cw + vw] = (raw * lax.rsqrt(power + NORM_EPS) * hgain * gate).astype(BF16)

    load_ao.wait()
    own = rows // 2
    my_rows = pl.ds(pl.multiple_of(tp * own, own), own)
    peer_rows = pl.ds(pl.multiple_of((1 - tp) * own, own), own)
    backs = []
    for i in range(OUT_CHUNKS):
        c = slice(i * step, (i + 1) * step)
        back_s[i] = (
            oacc[peer_rows, c] + dot16(cat[peer_rows, cw:cw + vw], wout[cw:cw + vw, c])
        ).astype(BF16)
        backs.append(remote(back_s.at[i], back_r.at[i], 2 + i, partner))
        backs[-1].start()
    for i in range(OUT_CHUNKS):
        c = slice(i * step, (i + 1) * step)
        part = oacc[my_rows, c] + dot16(cat[my_rows, cw:cw + vw], wout[cw:cw + vw, c])
        backs[i].wait()
        out_ref[:, c] = (part + back_r[i].astype(F32)).astype(BF16)


def on_device(n, tokens, gain, wb, wc, wh, taps, wq, wk, wv, wf, wg, bias, extra, init,
              hgain, wco, wao):
    rows = tokens.shape[0]
    feats = gain.shape[0]
    heads, dk, dv = init.shape
    cw = wb.shape[1]
    qk, vw = heads * dk, heads * dv
    widths = tuple(w.shape[1] for w in (wf, wk, wv, wq, wc, wh, wb, wg))
    sizes = (rows, feats, heads, dk, dv, cw, widths)
    vm, hbm = pl.BlockSpec(memory_space=pltpu.VMEM), pl.BlockSpec(memory_space=pl.ANY)
    n_blocks = rows // BLOCK
    levels = max(len(radices(n)), 1)
    out_rows = rows // 2
    step = feats // OUT_CHUNKS
    n_sems = 8 + 4 * levels
    return pl.pallas_call(
        functools.partial(kernel, n, sizes),
        out_shape=jax.ShapeDtypeStruct((out_rows, feats), BF16),
        in_specs=[vm, vm, hbm, hbm, hbm, vm, hbm, hbm, hbm, hbm, hbm, vm, vm, vm, vm, hbm, hbm],
        out_specs=vm,
        scratch_shapes=[
            pltpu.VMEM((feats, sum(widths)), BF16),
            pltpu.VMEM((cw + vw, feats), BF16),
            pltpu.VMEM((rows, feats // 2), BF16),
            pltpu.VMEM((rows, feats // 2), BF16),
            pltpu.VMEM((rows, feats // 2), BF16),
            pltpu.VMEM((rows, sum(widths)), F32),
            pltpu.VMEM((rows, CHUNK), F32),
            pltpu.VMEM((rows, qk), F32),
            pltpu.VMEM((rows, feats), F32),
            pltpu.VMEM((rows, sum(widths)), BF16),
            pltpu.VMEM((rows, qk), BF16),
            pltpu.VMEM((rows, qk), BF16),
            pltpu.VMEM((rows, vw), F32),
            pltpu.VMEM((n_blocks, dv, qk), F32),
            pltpu.VMEM((n_blocks, 8, qk), F32),
            pltpu.VMEM((heads * BLOCK, qk), BF16),
            pltpu.VMEM((heads * BLOCK, vw), BF16),
            pltpu.VMEM((rows + 8, cw), F32),
            pltpu.VMEM((16, cw), BF16),
            pltpu.VMEM((16, cw), BF16),
            pltpu.VMEM((rows, cw + vw), BF16),
            pltpu.VMEM((levels, 4, dv + 16, qk), BF16),
            pltpu.VMEM((OUT_CHUNKS, out_rows, step), BF16),
            pltpu.VMEM((OUT_CHUNKS, out_rows, step), BF16),
            pltpu.SemaphoreType.DMA((18,)),
            pltpu.SemaphoreType.DMA((n_sems,)),
            pltpu.SemaphoreType.DMA((n_sems,)),
        ],
        compiler_params=pltpu.CompilerParams(
            collective_id=0, has_side_effects=True, vmem_limit_bytes=60 * 2**20
        ),
        name="mixer",
    )(
        tokens, gain.reshape(1, feats), wb, wc, wh, taps, wq, wk, wv, wf, wg,
        bias.reshape(1, qk), extra.T, init.reshape(qk, dv), hgain.reshape(1, dv), wco, wao,
    )


def solution(mesh):
    placed = (
        P("sp", "tp"), P(), P(None, "tp"), P(None, "tp"), P(None, "tp"), P(None, "tp"),
        P(None, "tp"), P(None, "tp"), P(None, "tp"), P(None, "tp"), P(None, "tp"),
        P("tp"), P("sp", "tp"), P("tp", None, None), P(), P("tp", None), P("tp", None),
    )
    return jax.shard_map(
        functools.partial(on_device, mesh.shape["sp"]), mesh=mesh, in_specs=placed,
        out_specs=P(("sp", "tp"), None), check_vma=False,
    )
```
